256 devices in a mesh: sp: 64 (over z, y, core), tp: 4 (over x).
Axes of the slice: x: 4, y: 4, z: 8, core: 2. Of those that a mesh axis runs over, the one named last changes fastest.
Arguments:
- query_rows: bfloat16 [20480, 1024], P('sp', 'tp'), may hold values from -6 to 6
- key_rows: bfloat16 [20480, 1024], P('sp', 'tp'), may hold values from -6 to 6
- value_rows: bfloat16 [20480, 1024], P('sp', 'tp'), may hold values from -6 to 6
- key_shift: bfloat16 [20480, 16], P('sp', 'tp'), may hold values from -10 to 6
- documents: int32 [20480], P('sp'), may hold values from 0 to 31, never falling along the last dimension, each value on 1 to 1280 neighbouring positions
- out_weight: bfloat16 [1024, 2048], P('tp'), may hold values from -0.1875 to 0.1875
- stream: bfloat16 [20480, 2048], P('sp', 'tp'), may hold values from -8 to 8
- norm_gain: float32 [2048], replicated, may hold values from 0.1 to 1.9
- expert_ids: int32 [20480, 2], P('sp'), may hold values from 0 to 63, all different within a row; in each aligned block of 320 rows (0 to 319, 320 to 639, ...) at most 14 rows name the same one
- expert_weights: float32 [20480, 2], P('sp'), may hold values from 0.25 to 1
- gate_weight: bfloat16 [64, 2048, 3584], P('sp', None, 'tp'), may hold values from -0.125 to 0.125
- up_weight: bfloat16 [64, 2048, 3584], P('sp', None, 'tp'), may hold values from -0.125 to 0.125
- down_weight: bfloat16 [64, 3584, 2048], P('sp', 'tp'), may hold values from -0.09375 to 0.09375
Outputs:
- layer_out: bfloat16 [20480, 2048], P('sp', 'tp')
The draws below stay inside these ranges and needn't reach their ends.
Inputs may be any that keep to these rules, and one draw needn't show every extreme that they name: `expert_ids`: in each aligned block of 320 rows no expert is named by more than 14 rows, a bound that some block reaches; the entries of a row differ. `documents`: document numbers never fall along the positions; each document has 1 to 1280 positions, and one has exactly 1280.
All inputs are finite; a program needn't handle non-finite values.
Results may differ from the reference program's by a relative error of at most 0.013.
Values may be sent and summed in bfloat16 or wider, within the bound.
No kernel may reach another device: no remote copies, remote signals or barrier semaphores. Data moves between devices by JAX's collectives and lax.ppermute only.
A program may use at most 128 MiB of HBM per device.

```python
import math
import jax
import jax.numpy as jnp
import numpy as np
from jax import lax

D = 2048
HEADS = 16
HEAD = 64
FF = 3584
TOP_K = 2
REACH = 4
SHARD = 320
PACKED_TOKENS = 20480
EXPERTS = 64
CAP = 14
DOC_MOST = 1280
DOCS = 32
N_SP = 64
N_TP = 4


def draw_value_rows(key, part):
    noise_key, offset_key = jax.random.split(key)
    row_width = HEADS * HEAD
    noise_part = jax.random.normal(noise_key, (PACKED_TOKENS, row_width), jnp.float32)
    offset = jax.random.uniform(offset_key, (PACKED_TOKENS // SHARD, 1, row_width), jnp.float32, -1.5, 1.5)
    shifted = noise_part.reshape(PACKED_TOKENS // SHARD, SHARD, row_width) + offset
    return jnp.clip(shifted.reshape(PACKED_TOKENS, row_width), -6.0, 6.0).astype(jnp.bfloat16)


def draw_key_shift(key, part):
    random_children = jax.random.split(key, 6)
    slow_share = 0.5
    slow_heads = jax.random.uniform(random_children[0], (HEADS,), jnp.float32) < slow_share
    slow_level = jax.random.uniform(random_children[1], (HEADS,), jnp.float32, -8.0, -7.0)
    fast_level = jax.random.uniform(random_children[2], (HEADS,), jnp.float32, -4.0, -3.0)
    ground_level = jnp.where(slow_heads, slow_level, fast_level)
    shard_level = jax.random.uniform(random_children[3], (PACKED_TOKENS // SHARD, 1, 1), jnp.float32, -0.8, 0.8)
    portion_rows = jnp.broadcast_to(shard_level, (PACKED_TOKENS // SHARD, SHARD, 1)).reshape(PACKED_TOKENS, 1)
    spike_places = jax.random.randint(random_children[4], (8,), 0, PACKED_TOKENS)
    spike_mask = jnp.any(jnp.arange(PACKED_TOKENS)[:, None] == spike_places[None, :], axis=1)
    spike_rows = jnp.where(spike_mask, 6.5, 0.0)[:, None]
    coarse_estimate = 0.3 * jnp.clip(jax.random.normal(random_children[5], (PACKED_TOKENS, HEADS), jnp.float32), -3.0, 3.0)
    merged_output = ground_level[None, :] + portion_rows + spike_rows + coarse_estimate
    return jnp.clip(merged_output, -10.0, 6.0).astype(jnp.bfloat16)


def draw_stream(key, part):
    base_key, col_key = jax.random.split(key, 2)
    col_scale = jnp.exp(jnp.linspace(-0.916, 0.693, D)) * jax.random.uniform(col_key, (D,), jnp.float32, 0.7, 1.3)
    base_part = jax.random.normal(base_key, (PACKED_TOKENS, D), jnp.float32)
    return jnp.clip(base_part * col_scale[None, :], -8.0, 8.0).astype(jnp.bfloat16)


def block_scale(key, extent, cuts, low, high):
    def one(dim, shards_of):
        heights = jax.random.uniform(jax.random.fold_in(jax.random.fold_in(key, 6), dim), (shards_of,), jnp.float32, low / len(cuts), high / len(cuts))
        return jnp.repeat(jnp.exp(heights), extent[dim] // shards_of).reshape((-1,) + (1,) * (len(extent) - dim - 1))

    factor_of = one(*cuts[0])
    for cut in cuts[1:]:
        factor_of = factor_of * one(*cut)
    return factor_of


def length_profile(amount, total, reach, skew):
    portions = [(1 << 20) // math.isqrt(rank ** skew) + 1 for rank in range(2, amount + 1)]
    surplus, counts = total - reach - (amount - 1), [1] * (amount - 1)
    while surplus > 0:
        movable = [i for i in range(amount - 1) if counts[i] < reach]
        pool, left = sum([portions[i] for i in movable]), surplus
        for i in movable:
            extra = min(reach - counts[i], max(1, left * portions[i] // pool), surplus)
            counts[i] = counts[i] + extra
            surplus = surplus - extra
    return np.array([reach] + counts)


def ragged_sizes(own_key, count, total, limit, lean):
    if count == 2:
        one = jax.random.randint(own_key, (), max(1, total - limit), min(limit, total - 1) + 1)
        return jnp.stack([one, total - one])
    sizes = jnp.asarray(length_profile(count, total, limit, lean), jnp.int32)
    twos = (count - 1) // 2
    giver, receiver = sizes[1:1 + 2 * twos:2], sizes[2:2 + 2 * twos:2]
    room = jnp.minimum(giver - 1, limit - receiver)
    passed = jax.random.randint(jax.random.fold_in(own_key, 1), (twos,), 0, 1 << 20) % (room + 1)
    sizes = sizes.at[1:1 + 2 * twos:2].set(giver - passed).at[2:2 + 2 * twos:2].set(receiver + passed)
    return sizes[jax.random.permutation(jax.random.fold_in(own_key, 2), count)]


def shared_out(rng, own, number, rows, number_of, top, most, lean):
    sequence = jax.random.permutation(rng, number_of)
    packed, ordinary = portions_of(number_of, rows * top, most, lean, True), portions_of(number_of, rows * top, most, lean, False)
    places = jnp.arange(number_of)

    def named(tallies, rotation):
        used = int((tallies > 0).sum())
        fixed = max(1, used // 4)
        moved = fixed + (places - fixed + rotation * (used - fixed)) % max(1, number_of - fixed)
        return jnp.zeros((number_of,), jnp.int32).at[sequence[jnp.where(places < fixed, places, moved)]].set(jnp.asarray(tallies, jnp.int32))

    tallies = jnp.where(number % 4 == 0, named(packed, number // 4), named(ordinary, number - number // 4 - 1))
    mixed = jax.random.permutation(jax.random.fold_in(own, 3), number_of)
    giver, sink = mixed[0:number_of // 2 * 2:2], mixed[1:number_of // 2 * 2:2]
    slack = jnp.minimum(tallies[giver] - 1, most - tallies[sink]) // 2
    slack = jnp.where((giver == sequence[0]) | (sink == sequence[0]) | (tallies[sink] == 0), 0, jnp.maximum(slack, 0))
    moved = jax.random.randint(jax.random.fold_in(own, 4), (number_of // 2,), 0, 1 << 20) % (slack + 1)
    tallies = tallies.at[giver].add(-moved).at[sink].add(moved)
    labels = jnp.searchsorted(jnp.cumsum(tallies), jnp.arange(rows * top), side="right").astype(jnp.int32)
    listing = labels.reshape(top, rows).T
    listing = listing[jax.random.permutation(jax.random.fold_in(own, 1), rows)]
    rotation = jax.random.randint(jax.random.fold_in(own, 2), (rows, 1), 0, top)
    return jnp.take_along_axis(listing, (jnp.arange(top)[None, :] + rotation) % top, axis=1)


def portions_of(amount, total, limit, skew, full):
    loads = [(1 << 20) // math.isqrt(standing ** skew) + 1 for standing in range(1, amount + 1)]
    largest = limit if full else min(limit, max(-(-total // amount), total * loads[0] // sum(loads)))
    least = 1 if total - largest >= amount - 1 else 0
    holding, surplus = [largest] + [least] * (amount - 1), total - largest - least * (amount - 1)
    while surplus > 0:
        free = [i for i in range(1, amount) if holding[i] < largest] or [i for i in range(1, amount) if holding[i] < limit]
        mass, budget = sum([loads[i] for i in free]), surplus
        for i in free:
            addition = min(limit - holding[i], max(1, budget * loads[i] // mass), surplus)
            holding[i] = holding[i] + addition
            surplus = surplus - addition
    return np.array(holding)


def gaussian(key, extent, width, limit, cuts=(), kind=jnp.bfloat16):
    drawn = width * jax.random.normal(key, extent, jnp.float32)
    if cuts:
        drawn = drawn * block_scale(key, extent, cuts, -0.22, 0.18)
    return jnp.clip(drawn, -limit, limit).astype(kind)


def setup_inputs(seed: int = 0) -> dict:
    seeds = jax.random.split(jax.random.key(seed), 14)
    query_rows = gaussian(seeds[0], (PACKED_TOKENS, HEADS * HEAD), 1.0, 6.0, ((0, 64), (1, 4)))
    key_rows = gaussian(seeds[1], (PACKED_TOKENS, HEADS * HEAD), 1.0, 6.0, ((0, 64), (1, 4)))
    value_rows = draw_value_rows(jax.random.fold_in(seeds[13], 71), 0)
    key_shift = draw_key_shift(jax.random.fold_in(seeds[13], 71), 0)
    documents = jnp.searchsorted(jnp.cumsum(ragged_sizes(seeds[4], DOCS, PACKED_TOKENS, DOC_MOST, 2)), jnp.arange(PACKED_TOKENS), side="right").astype(jnp.int32)
    out_weight = gaussian(seeds[5], (HEADS * HEAD, D), (HEADS * HEAD) ** -0.5, 0.1875, ((0, 4),))
    stream = draw_stream(jax.random.fold_in(seeds[13], 71), 0)
    norm_gain = jnp.clip(1.0 + 0.18 * jax.random.normal(seeds[7], (D,), jnp.float32), 0.1, 1.9)
    expert_ids_keys = jax.random.split(jax.random.fold_in(seeds[8], 1), PACKED_TOKENS // SHARD)
    expert_ids_turns = jax.random.permutation(jax.random.fold_in(seeds[8], 3), PACKED_TOKENS // SHARD)
    expert_ids = jax.vmap(lambda own, number: shared_out(jax.random.fold_in(seeds[8], 2), own, number, SHARD, EXPERTS, TOP_K, CAP, 2))(expert_ids_keys, expert_ids_turns).reshape((PACKED_TOKENS, TOP_K))
    expert_weights = jnp.clip(0.25 + 0.75 * jax.random.uniform(seeds[9], (PACKED_TOKENS, TOP_K), jnp.float32) ** block_scale(seeds[9], (PACKED_TOKENS, TOP_K), ((0, 64),), -0.2, 0.2), 0.25, 1.0)
    gate_weight = gaussian(seeds[10], (EXPERTS, D, FF), D ** -0.5, 0.125, ((0, 64), (2, 4)))
    up_weight = gaussian(seeds[11], (EXPERTS, D, FF), D ** -0.5, 0.125, ((0, 64), (2, 4)))
    down_weight = gaussian(seeds[12], (EXPERTS, FF, D), FF ** -0.5, 0.09375, ((0, 64), (1, 4)))
    return {"query_rows": query_rows, "key_rows": key_rows, "value_rows": value_rows, "key_shift": key_shift, "documents": documents, "out_weight": out_weight, "stream": stream, "norm_gain": norm_gain, "expert_ids": expert_ids, "expert_weights": expert_weights, "gate_weight": gate_weight, "up_weight": up_weight, "down_weight": down_weight}


NORM_EPS = 1e-06

def reference(query_rows, key_rows, value_rows, key_shift, documents, out_weight, stream, norm_gain, expert_ids, expert_weights, gate_weight, up_weight, down_weight):
    front_pad = REACH * SHARD
    window = front_pad + SHARD
    query_heads = query_rows.astype(jnp.float32).reshape(PACKED_TOKENS, HEADS, HEAD)
    key_heads = jnp.pad(key_rows.astype(jnp.float32).reshape(PACKED_TOKENS, HEADS, HEAD), ((front_pad, 0), (0, 0), (0, 0)))
    value_heads = jnp.pad(value_rows.astype(jnp.float32).reshape(PACKED_TOKENS, HEADS, HEAD), ((front_pad, 0), (0, 0), (0, 0)))
    shift_pad = jnp.pad(key_shift.astype(jnp.float32), ((front_pad, 0), (0, 0)))
    doc_pad = jnp.pad(documents, (front_pad, 0), constant_values=-1)

    def attend_block(block_index):
        begin_row = (block_index * SHARD).astype(jnp.int32)
        query_block = lax.dynamic_slice_in_dim(query_heads, begin_row, SHARD, 0)
        query_docs = lax.dynamic_slice_in_dim(documents, begin_row, SHARD, 0)
        key_window = lax.dynamic_slice_in_dim(key_heads, begin_row, window, 0)
        value_window = lax.dynamic_slice_in_dim(value_heads, begin_row, window, 0)
        shift_window = lax.dynamic_slice_in_dim(shift_pad, begin_row, window, 0)
        key_docs = lax.dynamic_slice_in_dim(doc_pad, begin_row, window, 0)
        query_pos = begin_row + jnp.arange(SHARD, dtype=jnp.int32)
        key_pos = begin_row - front_pad + jnp.arange(window, dtype=jnp.int32)
        scores = jnp.einsum('qhd,khd->hqk', query_block, key_window) * HEAD ** (-0.5)
        scores = scores + jnp.transpose(shift_window)[:, None, :]
        admitted = (key_pos[None, :] < query_pos[:, None]) & (key_docs[None, :] == query_docs[:, None])
        log_rest = jnp.where(admitted[None], jax.nn.log_sigmoid(-scores), 0.0)
        log_after = lax.cumsum(log_rest, axis=2, reverse=True) - log_rest
        stick_weight = jnp.where(admitted[None], jnp.exp(jax.nn.log_sigmoid(scores) + log_after), 0.0).astype(jnp.bfloat16)
        stick_weight = lax.optimization_barrier(stick_weight).astype(jnp.float32)
        attended = jnp.einsum('hqk,khd->qhd', stick_weight, value_window)
        return attended.reshape(SHARD, HEADS * HEAD).astype(jnp.bfloat16)
    attended = lax.map(attend_block, jnp.arange(N_SP, dtype=jnp.int32)).reshape(PACKED_TOKENS, HEADS * HEAD)
    group_width = HEADS * HEAD // N_TP
    projected = jnp.zeros((PACKED_TOKENS, D), jnp.float32)
    for part_index in range(N_TP):
        lower = part_index * group_width
        partial_value = jnp.dot(attended[:, lower:lower + group_width], out_weight[lower:lower + group_width], preferred_element_type=jnp.float32)
        projected = projected + lax.optimization_barrier(partial_value.astype(jnp.bfloat16)).astype(jnp.float32)
    middle = (stream.astype(jnp.float32) + projected).astype(jnp.bfloat16)
    middle_wide = lax.optimization_barrier(middle).astype(jnp.float32)
    inv_rms = lax.rsqrt(lax.optimization_barrier(jnp.mean(middle_wide * middle_wide, axis=1, keepdims=True)) + NORM_EPS)
    normed = (middle_wide * inv_rms * norm_gain[None, :]).astype(jnp.bfloat16)
    flat_ids = expert_ids.reshape(N_SP, SHARD * TOP_K).astype(jnp.int32)
    onehot = (flat_ids[:, :, None] == jnp.arange(EXPERTS, dtype=jnp.int32)[None, None, :]).astype(jnp.int32)
    slot_index = lax.optimization_barrier(jnp.sum((jnp.cumsum(onehot, axis=1) - 1) * onehot, axis=2)).astype(jnp.int32)
    source = jnp.broadcast_to(jnp.arange(N_SP, dtype=jnp.int32)[:, None], flat_ids.shape)
    token_index = source * SHARD + jnp.arange(SHARD * TOP_K, dtype=jnp.int32)[None, :] // TOP_K
    table = jnp.zeros((EXPERTS, N_SP, CAP), jnp.int32).at[flat_ids, source, slot_index].set(token_index)
    filled = jnp.zeros((EXPERTS, N_SP, CAP), jnp.int32).at[flat_ids, source, slot_index].set(1)
    hidden_group = FF // N_TP

    def run_expert(expert_index):
        row_index = table[expert_index].reshape(N_SP * CAP)
        used = filled[expert_index].reshape(N_SP * CAP, 1) > 0
        row_block = jnp.where(used, normed[row_index], jnp.zeros((), jnp.bfloat16))
        gate_value = jnp.dot(row_block, gate_weight[expert_index], preferred_element_type=jnp.float32)
        up_value = jnp.dot(row_block, up_weight[expert_index], preferred_element_type=jnp.float32)
        hidden = (jax.nn.silu(gate_value) * up_value).astype(jnp.bfloat16)
        summed = jnp.zeros((N_SP * CAP, D), jnp.float32)
        for part_index in range(N_TP):
            lower = part_index * hidden_group
            partial_value = jnp.dot(hidden[:, lower:lower + hidden_group], down_weight[expert_index, lower:lower + hidden_group], preferred_element_type=jnp.float32)
            summed = summed + lax.optimization_barrier(partial_value.astype(jnp.bfloat16)).astype(jnp.float32)
        return summed.astype(jnp.bfloat16)
    expert_out = lax.map(run_expert, jnp.arange(EXPERTS, dtype=jnp.int32))
    flat_pos = (flat_ids * (N_SP * CAP) + source * CAP + slot_index).reshape(PACKED_TOKENS * TOP_K)
    picked = expert_out.reshape(EXPERTS * N_SP * CAP, D)[flat_pos].astype(jnp.float32).reshape(PACKED_TOKENS, TOP_K, D)
    mixed = lax.optimization_barrier(jnp.sum(picked * expert_weights[:, :, None], axis=1))
    return (middle_wide + mixed).astype(jnp.bfloat16)
```

```python
import functools

import jax
import jax.numpy as jnp
from jax import lax
from jax.experimental import pallas as pl
from jax.experimental.pallas import tpu as pltpu
from jax.sharding import PartitionSpec as P


D = 2048
HEAD = 64
NORM_EPS = 1e-06
EXTRA = 16
LOG2E = 1.4426950408889634
F32 = jnp.float32
BF16 = jnp.bfloat16


def shifted(x, axis, by):
    size = lax.axis_size(axis)
    return lax.ppermute(x, axis, [(i, i + by) for i in range(size) if 0 <= i + by < size])


def rotated(x, axis, by):
    size = lax.axis_size(axis)
    return lax.ppermute(x, axis, [(i, (i + by) % size) for i in range(size)])


def attend_body(own, last, heads, *refs):
    if last:
        *refs, shift_scr, blk_scr, acc_ref, tot_ref = refs
        refs = (*refs, acc_ref, tot_ref)
    else:
        *refs, shift_scr, blk_scr = refs
    if own:
        q_ref, blk_ref, tri_ref, qdoc_ref, acc_ref, tot_ref = refs
    elif last:
        *refs, acc_ref, tot_ref = refs
        q_ref, near_ref, far_ref, tri_ref, qdoc_ref, acc_in, tot_in, done_ref = refs
    else:
        q_ref, near_ref, far_ref, tri_ref, qdoc_ref, acc_in, tot_in, acc_ref, tot_ref = refs
    rows = q_ref.shape[0]
    keys = shift_scr.shape[1]
    width = heads * HEAD
    groups = [(lo, min(keys, lo + 128)) for lo in range(0, keys, 128)]
    lane = lax.broadcasted_iota(jnp.int32, (rows, 128), 1)

    def one_head(blk, admitted, acc_old, tot_old, head):
        pair = head // 2
        cols = pl.ds(pl.multiple_of(128 * pair, 128), 128)
        v_cols = pl.ds(pl.multiple_of(width + 128 * pair, 128), 128)
        tot_cols = pl.ds(pl.multiple_of(128 * head, 128), 128)
        mine = (lane >= HEAD) == (head % 2 == 1)
        q_head = jnp.where(mine, q_ref[:, cols].astype(F32), 0.0).astype(BF16)
        later = None if tot_old is None else tot_old[:, tot_cols]
        shift = shift_scr[pl.ds(head, 1), :]
        scores = lax.dot_general(q_head, blk[0:keys, cols], (((1,), (1,)), ((), ())), preferred_element_type=F32)
        sticks = []
        for (lo, hi), ok in reversed(list(zip(groups, admitted))):
            size = hi - lo
            s = scores[:, lo:hi] * (LOG2E * HEAD ** (-0.5)) + shift[:, lo:hi]
            drop = jnp.maximum(s, 0.0) + jnp.log2(1.0 + jnp.exp2(-jnp.abs(s)))
            rest = jnp.where(ok, drop, 0.0)
            high = rest.astype(BF16)
            low = (rest - high.astype(F32)).astype(BF16)
            if size == 128:
                sums = jnp.dot(jnp.concatenate([high, low], axis=1), tri_ref[...], preferred_element_type=F32)
            else:
                sums = jnp.dot(high, tri_ref[0:size], preferred_element_type=F32) + jnp.dot(
                    low, tri_ref[0:size], preferred_element_type=F32
                )
            z = (s - drop) + sums[:, 0:size]
            if later is not None:
                z = z + later[:, 0:size]
            sticks.append(jnp.where(ok, jnp.exp2(z), 0.0).astype(BF16))
            gone = sums[:, 128:256]
            later = gone if later is None else later + gone
        stick = jnp.concatenate(sticks[::-1], axis=1)
        out = jnp.dot(stick, blk[0:keys, v_cols], preferred_element_type=F32)
        tot_ref[:, tot_cols] = later
        old = 0.0 if acc_old is None else acc_old[:, cols]
        acc_ref[:, cols] = old + jnp.where(mine, out, 0.0)

    def one_block(blk, acc_old, tot_old):
        extra = blk[keys : keys + EXTRA, 0:keys].astype(F32)
        shift_scr[...] = extra * LOG2E
        admitted = []
        for lo, hi in groups:
            ok = extra[heads : heads + 1, lo:hi] == qdoc_ref[...]
            if own:
                q_iota = lax.broadcasted_iota(jnp.int32, (rows, hi - lo), 0)
                k_iota = lax.broadcasted_iota(jnp.int32, (rows, hi - lo), 1) + lo
                ok = ok & (k_iota < q_iota)
            admitted.append(ok)
        lax.fori_loop(0, heads, lambda h, _: (one_head(blk, admitted, acc_old, tot_old, h), 0)[1], 0)

    if own:
        acc_ref[...] = jnp.zeros_like(acc_ref)
        one_block(blk_ref, acc_ref, None)
    else:
        acc_ref[...] = acc_in[...]
        tot_ref[...] = tot_in[...]

        def visit(t, _):
            @pl.when(t == 0)
            def _():
                blk_scr[...] = near_ref[...]

            @pl.when(t == 1)
            def _():
                blk_scr[...] = far_ref[...]

            one_block(blk_scr, acc_ref, tot_ref)
            return 0

        lax.fori_loop(0, 2, visit, 0)
        if last:
            done_ref[...] = acc_ref[...].astype(BF16)


def attend(own, last, heads, q, blks, tri, qdoc, state):
    rows = q.shape[0]
    outs = [
        jax.ShapeDtypeStruct((rows, heads * HEAD), F32),
        jax.ShapeDtypeStruct((rows, heads * 128), F32),
    ]
    scratch = []
    if last:
        scratch = [pltpu.VMEM(o.shape, o.dtype) for o in outs]
        outs = [jax.ShapeDtypeStruct((rows, heads * HEAD), BF16)]
    keys = blks[0].shape[0] - EXTRA
    return pl.pallas_call(
        functools.partial(attend_body, own, last, heads),
        out_shape=outs,
        scratch_shapes=[pltpu.VMEM((EXTRA, keys), F32), pltpu.VMEM(blks[0].shape, BF16)] + scratch,
        name="attend_own" if own else "attend_visit",
        cost_estimate=pl.CostEstimate(
            flops=len(blks) * 2 * heads * rows * keys * (2 * HEAD + 2 * keys),
            transcendentals=len(blks) * 3 * heads * rows * keys,
            bytes_accessed=2 * blks[0].size * len(blks) + 4 * rows * heads * HEAD,
        ),
        compiler_params=pltpu.CompilerParams(vmem_limit_bytes=24 << 20),
    )(q, *blks, tri, qdoc, *state)


def expert_body(
    take_ref, own, left, right, opp_t, opp_b, gain, gate_w, up_w, down_w,
    out_ft, out_fb, out_up, out_down, out_own, norm, g_acc, hid, gate_v, up_v, down_v, sems,
):
    half = opp_t.shape[0]
    cols = own.shape[1]

    def fetches(i):
        rows = pl.ds(pl.multiple_of(take_ref[i] * cols, cols), cols)
        lanes = pl.ds(pl.multiple_of(take_ref[4 + i] * cols, cols), cols)
        return (
            pltpu.make_async_copy(gate_w.at[0, rows], gate_v.at[i], sems.at[0, i]),
            pltpu.make_async_copy(up_w.at[0, rows], up_v.at[i], sems.at[1, i]),
            pltpu.make_async_copy(down_w.at[0, :, lanes], down_v.at[i], sems.at[2, i]),
        )

    for kind in range(3):
        for i in range(4):
            fetches(i)[kind].start()

    def whole(kind):
        for i in range(4):
            fetches(i)[kind].wait()

    for base, opp in ((0, opp_t), (half, opp_b)):

        def normed(t, _, base=base, opp=opp):
            here = pl.ds(pl.multiple_of(base + 32 * t, 32), 32)
            there = pl.ds(pl.multiple_of(32 * t, 32), 32)
            wide = [r.astype(F32) for r in (own[here], left[here], right[here], opp[there])]
            total = sum(jnp.sum(w * w, axis=1, keepdims=True) for w in wide)
            inv = lax.rsqrt(total / D + NORM_EPS)
            for i in range(4):
                norm[i, here] = (wide[i] * inv * gain[take_ref[i]]).astype(BF16)
            return 0

        lax.fori_loop(0, half // 32, normed, 0)
    whole(0)
    g_acc[...] = sum(jnp.dot(norm[i], gate_v[i], preferred_element_type=F32) for i in range(4))
    whole(1)
    u = sum(jnp.dot(norm[i], up_v[i], preferred_element_type=F32) for i in range(4))
    g = g_acc[...]
    hid[...] = (g / (1.0 + jnp.exp(-g)) * u).astype(BF16)
    whole(2)

    def down(i, _):
        norm[i] = jnp.dot(hid[...], down_v[i], preferred_element_type=F32).astype(BF16)
        return 0

    lax.fori_loop(0, 4, down, 0)
    out_ft[...] = norm[0, :half]
    out_fb[...] = norm[0, half:]
    out_up[...] = norm[1]
    out_down[...] = norm[2]
    out_own[...] = norm[3]


def experts_of(take, own, left, right, opp_t, opp_b, gain, gate_w, up_w, down_w):
    rows, cols = own.shape
    hidden = gate_w.shape[2]
    smem = pl.BlockSpec(memory_space=pltpu.SMEM)
    vmem = pl.BlockSpec(memory_space=pltpu.VMEM)
    hbm = pl.BlockSpec(memory_space=pltpu.HBM)
    shape = lambda r: jax.ShapeDtypeStruct((r, cols), BF16)
    return pl.pallas_call(
        expert_body,
        out_shape=[shape(rows // 2), shape(rows // 2), shape(rows), shape(rows), shape(rows)],
        in_specs=[smem] + [vmem] * 6 + [hbm] * 3,
        out_specs=[vmem] * 5,
        scratch_shapes=[
            pltpu.VMEM((4, rows, cols), BF16),
            pltpu.VMEM((rows, hidden), F32),
            pltpu.VMEM((rows, hidden), BF16),
            pltpu.VMEM((4, cols, hidden), BF16),
            pltpu.VMEM((4, cols, hidden), BF16),
            pltpu.VMEM((4, hidden, cols), BF16),
            pltpu.SemaphoreType.DMA((3, 4)),
        ],
        name="experts",
        cost_estimate=pl.CostEstimate(
            flops=6 * rows * 4 * cols * hidden,
            transcendentals=rows * hidden,
            bytes_accessed=2 * 12 * cols * hidden + 16 * rows * cols,
        ),
        compiler_params=pltpu.CompilerParams(vmem_limit_bytes=48 << 20),
    )(take, own, left, right, opp_t, opp_b, gain, gate_w, up_w, down_w)


def gather_tp(x):
    half = x.shape[0] // 2
    left = rotated(x, "tp", 1)
    right = rotated(x, "tp", -1)
    opp_t = rotated(left[:half], "tp", 1)
    opp_b = rotated(right[half:], "tp", -1)
    return left, right, opp_t, opp_b


def scatter_sum_tp(parts, shape):
    far_t, far_b, up, down, own = parts
    half = far_t.shape[0]
    from_left = rotated(far_t, "tp", 1)
    from_right = rotated(far_b, "tp", -1)
    add = lambda a, b: (a.astype(F32) + b.astype(F32)).astype(BF16)
    up = lax.dynamic_update_slice(up, add(up[:half], from_left), (0, 0))
    down = lax.dynamic_update_slice(down, add(down[half:], from_right), (half, 0))
    a = rotated(up, "tp", 1)
    b = rotated(down, "tp", -1)
    return (own.astype(F32) + a.astype(F32) + b.astype(F32)).astype(BF16).reshape(shape)


def layer(
    query_rows,
    key_rows,
    value_rows,
    key_shift,
    documents,
    out_weight,
    stream,
    norm_gain,
    expert_ids,
    expert_weights,
    gate_weight,
    up_weight,
    down_weight,
):
    rows, width = query_rows.shape
    heads = key_shift.shape[1]
    cols = stream.shape[1]
    me = lax.axis_index("tp")

    doc = (documents + 1).astype(F32)
    extra = jnp.concatenate(
        [jnp.transpose(key_shift), doc[None].astype(BF16), jnp.zeros((EXTRA - heads - 1, rows), BF16)], axis=0
    )
    extra = jnp.pad(extra, ((0, 0), (0, 2 * width - rows)))
    packed = jnp.concatenate([jnp.concatenate([key_rows, value_rows], axis=1), extra], axis=0)
    odd = lax.rem(lax.axis_index("sp"), 2) == 1
    size = lax.axis_size("sp")
    swap = lambda x: lax.ppermute(x, "sp", [(i, i ^ 1) for i in range(size)])
    two = shifted(packed, "sp", 2)
    four = shifted(two, "sp", 2)
    one = swap(jnp.where(odd, two, packed))
    held = lax.optimization_barrier((two, one))[0]
    three = swap(jnp.where(odd, four, held))

    cut = lambda k: lax.dynamic_slice_in_dim(out_weight, lax.rem(me + k, 4) * cols, cols, axis=1)
    w_own = cut(0)
    w_left = rotated(cut(1), "tp", 1)
    w_right = rotated(cut(3), "tp", -1)
    w_opp = rotated(cut(2), "tp", 2)

    qdoc = doc[:, None]
    iota = jnp.arange(rows, dtype=jnp.int32)
    later = (iota[:, None] > iota[None, :]).astype(BF16)
    lanes = jnp.arange(128, dtype=jnp.int32)
    tri = jnp.where(lanes[:, None] > lanes[None, :], -1.0, 0.0)
    tri = jnp.concatenate([tri, jnp.full((128, 128), -1.0)], axis=1).astype(BF16)
    tri = jnp.concatenate([tri, tri], axis=0)
    state = attend(True, False, heads, query_rows, (packed,), tri, qdoc, ())
    state = attend(False, False, heads, query_rows, (one, two), tri, qdoc, state)
    state = attend(False, True, heads, query_rows, (three, four), tri, qdoc, state)
    attended = state[0]

    top = expert_ids.shape[1]
    experts = size * gate_weight.shape[0]
    capacity = (4 * rows * top + 3 * experts - 1) // (3 * experts)
    e_iota = jnp.arange(experts, dtype=jnp.int32)[None, :]
    chosen = [(expert_ids[:, k : k + 1] == e_iota) for k in range(top)]
    count = sum(c.astype(BF16) for c in chosen)
    earlier = jnp.dot(later, count, preferred_element_type=F32)
    ids = [expert_ids[:, k : k + 1] for k in range(top)]
    slot = [jnp.sum(jnp.where(c, earlier, 0.0), axis=1, keepdims=True).astype(jnp.int32) for c in chosen]
    targets = jnp.arange(experts * capacity, dtype=jnp.int32)[None]
    select = sum((i * capacity + s == targets).astype(BF16) for i, s in zip(ids, slot))

    left, right, opp_t, opp_b = gather_tp(attended)
    opp = jnp.concatenate([opp_t, opp_b], axis=0)
    part = lambda a, w: jnp.dot(a, w, preferred_element_type=F32).astype(BF16).astype(F32)
    projected = part(attended, w_own) + part(left, w_left) + part(right, w_right) + part(opp, w_opp)
    middle = (stream.astype(F32) + projected).astype(BF16)

    send = lax.dot_general(select, middle, (((0,), (0,)), ((), ())), preferred_element_type=F32)
    send = send.astype(BF16).reshape(experts, capacity, cols)
    block = lax.all_to_all(send, "sp", 0, 0, tiled=True)
    take = lax.rem(jnp.array([0, 3, 1, 2, 2, 1, 3, 0], jnp.int32) + me, 4)
    gain = norm_gain.reshape(4, 1, cols)
    mixed = middle.astype(F32)
    for lo, hi in ((8, capacity), (0, 8)):
        items = hi - lo
        part = block[:, lo:hi].reshape(experts * items, cols)
        wide = gather_tp(part)
        parts = experts_of(take, part, *wide, gain, gate_weight, up_weight, down_weight)
        result = scatter_sum_tp(parts, (experts, items, cols))
        back = lax.all_to_all(result, "sp", 0, 0, tiled=True).reshape(experts * items, cols)

        slots = jnp.arange(experts * items, dtype=jnp.int32)[None]
        for k in range(top):
            place = jnp.where((slot[k] >= lo) & (slot[k] < hi), ids[k] * items + slot[k] - lo, -1)
            value = jnp.dot((place == slots).astype(BF16), back, preferred_element_type=F32)
            mixed = mixed + value * expert_weights[:, k : k + 1]
    return mixed.astype(BF16)


def solution(mesh):
    in_specs = (
        P("sp", "tp"),
        P("sp", "tp"),
        P("sp", "tp"),
        P("sp", "tp"),
        P("sp"),
        P("tp", None),
        P("sp", "tp"),
        P(),
        P("sp", None),
        P("sp", None),
        P("sp", None, "tp"),
        P("sp", None, "tp"),
        P("sp", "tp", None),
    )
    out_specs = P("sp", "tp")
    return jax.shard_map(layer, mesh=mesh, in_specs=in_specs, out_specs=out_specs, check_vma=False)
```

```python
import functools

import jax
import jax.numpy as jnp
from jax import lax
from jax.experimental import pallas as pl
from jax.experimental.pallas import tpu as pltpu
from jax.sharding import PartitionSpec as P


D = 2048
HEAD = 64
NORM_EPS = 1e-06
EXTRA = 16
LOG2E = 1.4426950408889634
F32 = jnp.float32
BF16 = jnp.bfloat16


def shifted(x, axis, by):
    size = lax.axis_size(axis)
    return lax.ppermute(x, axis, [(i, i + by) for i in range(size) if 0 <= i + by < size])


def rotated(x, axis, by):
    size = lax.axis_size(axis)
    return lax.ppermute(x, axis, [(i, (i + by) % size) for i in range(size)])


def attend_body(own, last, heads, *refs):
    if last:
        *refs, bias_scr, shift_scr, blk_scr, acc_ref, tot_ref = refs
        refs = (*refs, acc_ref, tot_ref)
    else:
        *refs, bias_scr, shift_scr, blk_scr = refs
    if own:
        q_ref, blk_ref, tri_ref, qdoc_ref, acc_ref, tot_ref = refs
    elif last:
        *refs, acc_ref, tot_ref = refs
        q_ref, near_ref, far_ref, tri_ref, qdoc_ref, acc_in, tot_in, done_ref = refs
    else:
        q_ref, near_ref, far_ref, tri_ref, qdoc_ref, acc_in, tot_in, acc_ref, tot_ref = refs
    rows = q_ref.shape[0]
    keys = shift_scr.shape[1]
    width = heads * HEAD
    groups = [(lo, min(keys, lo + 128)) for lo in range(0, keys, 128)]
    lane = lax.broadcasted_iota(jnp.int32, (rows, 128), 1)

    def one_head(blk, acc_old, tot_old, head):
        pair = head // 2
        cols = pl.ds(pl.multiple_of(128 * pair, 128), 128)
        v_cols = pl.ds(pl.multiple_of(width + 128 * pair, 128), 128)
        tot_cols = pl.ds(pl.multiple_of(128 * head, 128), 128)
        mine = (lane >= HEAD) == (head % 2 == 1)
        q_head = jnp.where(mine, q_ref[:, cols].astype(F32), 0.0).astype(BF16)
        later = None if tot_old is None else tot_old[:, tot_cols]
        shift = shift_scr[pl.ds(head, 1), :]
        scores = lax.dot_general(q_head, blk[0:keys, cols], (((1,), (1,)), ((), ())), preferred_element_type=F32)
        sticks = []
        for lo, hi in reversed(groups):
            size = hi - lo
            s = scores[:, lo:hi] * (LOG2E * HEAD ** (-0.5)) + shift[:, lo:hi] + bias_scr[:, lo:hi]
            drop = jnp.maximum(s, 0.0) + jnp.log2(1.0 + jnp.exp2(-jnp.abs(s)))
            high = drop.astype(BF16)
            low = (drop - high.astype(F32)).astype(BF16)
            if size == 128:
                sums = jnp.dot(jnp.concatenate([high, low], axis=1), tri_ref[...], preferred_element_type=F32)
            else:
                sums = jnp.dot(high, tri_ref[0:size], preferred_element_type=F32) + jnp.dot(
                    low, tri_ref[0:size], preferred_element_type=F32
                )
            z = s + sums[:, 0:size]
            if later is not None:
                z = z + later[:, 0:size]
            sticks.append(jnp.exp2(z).astype(BF16))
            gone = sums[:, 128:256]
            later = gone if later is None else later + gone
        stick = jnp.concatenate(sticks[::-1], axis=1)
        out = jnp.dot(stick, blk[0:keys, v_cols], preferred_element_type=F32)
        tot_ref[:, tot_cols] = later
        old = 0.0 if acc_old is None else acc_old[:, cols]
        acc_ref[:, cols] = old + jnp.where(mine, out, 0.0)

    def one_block(blk, acc_old, tot_old):
        extra = blk[keys : keys + EXTRA, 0:keys].astype(F32)
        shift_scr[...] = extra * LOG2E
        ok = extra[heads : heads + 1, :] == qdoc_ref[...]
        if own:
            q_iota = lax.broadcasted_iota(jnp.int32, (rows, keys), 0)
            k_iota = lax.broadcasted_iota(jnp.int32, (rows, keys), 1)
            ok = ok & (k_iota < q_iota)
        bias_scr[...] = jnp.where(ok, 0.0, -1e30)
        lax.fori_loop(0, heads, lambda h, _: (one_head(blk, acc_old, tot_old, h), 0)[1], 0)

    if own:
        acc_ref[...] = jnp.zeros_like(acc_ref)
        one_block(blk_ref, acc_ref, None)
    else:
        acc_ref[...] = acc_in[...]
        tot_ref[...] = tot_in[...]

        def copy_rows(ref, r):
            here = pl.ds(pl.multiple_of(48 * r, 48), 48)
            blk_scr[here] = ref[here]

        def visit(t, _):
            for n, ref in enumerate((near_ref, far_ref)):

                @pl.when(t == n)
                def _(ref=ref):
                    lax.fori_loop(0, ref.shape[0] // 48, lambda r, _: (copy_rows(ref, r), 0)[1], 0)

            one_block(blk_scr, acc_ref, tot_ref)
            return 0

        lax.fori_loop(0, 2, visit, 0)
        if last:
            done_ref[...] = acc_ref[...].astype(BF16)


def attend(own, last, heads, q, blks, tri, qdoc, state):
    rows = q.shape[0]
    outs = [
        jax.ShapeDtypeStruct((rows, heads * HEAD), F32),
        jax.ShapeDtypeStruct((rows, heads * 128), F32),
    ]
    scratch = []
    if last:
        scratch = [pltpu.VMEM(o.shape, o.dtype) for o in outs]
        outs = [jax.ShapeDtypeStruct((rows, heads * HEAD), BF16)]
    keys = blks[0].shape[0] - EXTRA
    return pl.pallas_call(
        functools.partial(attend_body, own, last, heads),
        out_shape=outs,
        scratch_shapes=[pltpu.VMEM((rows, keys), F32), pltpu.VMEM((EXTRA, keys), F32), pltpu.VMEM(blks[0].shape, BF16)] + scratch,
        name="attend_own" if own else "attend_visit",
        cost_estimate=pl.CostEstimate(
            flops=len(blks) * 2 * heads * rows * keys * (2 * HEAD + 2 * keys),
            transcendentals=len(blks) * 3 * heads * rows * keys,
            bytes_accessed=2 * blks[0].size * len(blks) + 4 * rows * heads * HEAD,
        ),
        compiler_params=pltpu.CompilerParams(vmem_limit_bytes=24 << 20),
    )(q, *blks, tri, qdoc, *state)


def expert_body(
    take_ref, own, left, right, opp_t, opp_b, gain, gate_w, up_w, down_w,
    out_ft, out_fb, out_up, out_down, out_own, norm, g_acc, hid, gate_v, up_v, down_v, sems,
):
    half = opp_t.shape[0]
    cols = own.shape[1]

    def fetches(i):
        rows = pl.ds(pl.multiple_of(take_ref[i] * cols, cols), cols)
        lanes = pl.ds(pl.multiple_of(take_ref[4 + i] * cols, cols), cols)
        return (
            pltpu.make_async_copy(gate_w.at[0, rows], gate_v.at[i], sems.at[0, i]),
            pltpu.make_async_copy(up_w.at[0, rows], up_v.at[i], sems.at[1, i]),
            pltpu.make_async_copy(down_w.at[0, :, lanes], down_v.at[i], sems.at[2, i]),
        )

    for kind in range(3):
        for i in range(4):
            fetches(i)[kind].start()

    def whole(kind):
        for i in range(4):
            fetches(i)[kind].wait()

    for base, opp in ((0, opp_t), (half, opp_b)):

        def normed(t, _, base=base, opp=opp):
            here = pl.ds(pl.multiple_of(base + 32 * t, 32), 32)
            there = pl.ds(pl.multiple_of(32 * t, 32), 32)
            wide = [r.astype(F32) for r in (own[here], left[here], right[here], opp[there])]
            total = sum(jnp.sum(w * w, axis=1, keepdims=True) for w in wide)
            inv = lax.rsqrt(total / D + NORM_EPS)
            for i in range(4):
                norm[i, here] = (wide[i] * inv * gain[take_ref[i]]).astype(BF16)
            return 0

        lax.fori_loop(0, half // 32, normed, 0)
    whole(0)
    g_acc[...] = sum(jnp.dot(norm[i], gate_v[i], preferred_element_type=F32) for i in range(4))
    whole(1)
    u = sum(jnp.dot(norm[i], up_v[i], preferred_element_type=F32) for i in range(4))
    g = g_acc[...]
    hid[...] = (g / (1.0 + jnp.exp(-g)) * u).astype(BF16)
    whole(2)

    def down(i, _):
        norm[i] = jnp.dot(hid[...], down_v[i], preferred_element_type=F32).astype(BF16)
        return 0

    lax.fori_loop(0, 4, down, 0)

    def spread(t, _):
        top = pl.ds(pl.multiple_of(32 * t, 32), 32)
        low = pl.ds(pl.multiple_of(half + 32 * t, 32), 32)
        out_ft[top] = norm[0, top]
        out_fb[top] = norm[0, low]
        for rows in (top, low):
            out_up[rows] = norm[1, rows]
            out_down[rows] = norm[2, rows]
            out_own[rows] = norm[3, rows]
        return 0

    lax.fori_loop(0, half // 32, spread, 0)


def experts_of(take, own, left, right, opp_t, opp_b, gain, gate_w, up_w, down_w):
    rows, cols = own.shape
    hidden = gate_w.shape[2]
    smem = pl.BlockSpec(memory_space=pltpu.SMEM)
    vmem = pl.BlockSpec(memory_space=pltpu.VMEM)
    hbm = pl.BlockSpec(memory_space=pltpu.HBM)
    shape = lambda r: jax.ShapeDtypeStruct((r, cols), BF16)
    return pl.pallas_call(
        expert_body,
        out_shape=[shape(rows // 2), shape(rows // 2), shape(rows), shape(rows), shape(rows)],
        in_specs=[smem] + [vmem] * 6 + [hbm] * 3,
        out_specs=[vmem] * 5,
        scratch_shapes=[
            pltpu.VMEM((4, rows, cols), BF16),
            pltpu.VMEM((rows, hidden), F32),
            pltpu.VMEM((rows, hidden), BF16),
            pltpu.VMEM((4, cols, hidden), BF16),
            pltpu.VMEM((4, cols, hidden), BF16),
            pltpu.VMEM((4, hidden, cols), BF16),
            pltpu.SemaphoreType.DMA((3, 4)),
        ],
        name="experts",
        cost_estimate=pl.CostEstimate(
            flops=6 * rows * 4 * cols * hidden,
            transcendentals=rows * hidden,
            bytes_accessed=2 * 12 * cols * hidden + 16 * rows * cols,
        ),
        compiler_params=pltpu.CompilerParams(vmem_limit_bytes=48 << 20),
    )(take, own, left, right, opp_t, opp_b, gain, gate_w, up_w, down_w)


def gather_tp(x):
    half = x.shape[0] // 2
    left = rotated(x, "tp", 1)
    right = rotated(x, "tp", -1)
    opp_t = rotated(left[:half], "tp", 1)
    opp_b = rotated(right[half:], "tp", -1)
    return left, right, opp_t, opp_b


def scatter_sum_tp(parts, shape):
    far_t, far_b, up, down, own = parts
    half = far_t.shape[0]
    from_left = rotated(far_t, "tp", 1)
    from_right = rotated(far_b, "tp", -1)
    add = lambda a, b: (a.astype(F32) + b.astype(F32)).astype(BF16)
    up = lax.dynamic_update_slice(up, add(up[:half], from_left), (0, 0))
    down = lax.dynamic_update_slice(down, add(down[half:], from_right), (half, 0))
    a = rotated(up, "tp", 1)
    b = rotated(down, "tp", -1)
    return (own.astype(F32) + a.astype(F32) + b.astype(F32)).astype(BF16).reshape(shape)


def layer(
    query_rows,
    key_rows,
    value_rows,
    key_shift,
    documents,
    out_weight,
    stream,
    norm_gain,
    expert_ids,
    expert_weights,
    gate_weight,
    up_weight,
    down_weight,
):
    rows, width = query_rows.shape
    heads = key_shift.shape[1]
    cols = stream.shape[1]
    me = lax.axis_index("tp")

    doc = (documents + 1).astype(F32)
    extra = jnp.concatenate(
        [jnp.transpose(key_shift), doc[None].astype(BF16), jnp.zeros((EXTRA - heads - 1, rows), BF16)], axis=0
    )
    extra = jnp.pad(extra, ((0, 0), (0, 2 * width - rows)))
    packed = jnp.concatenate([jnp.concatenate([key_rows, value_rows], axis=1), extra], axis=0)
    odd = lax.rem(lax.axis_index("sp"), 2) == 1
    size = lax.axis_size("sp")
    swap = lambda x: lax.ppermute(x, "sp", [(i, i ^ 1) for i in range(size)])
    two = shifted(packed, "sp", 2)
    four = shifted(packed, "sp", 4)
    one = swap(jnp.where(odd, two, packed))
    held = lax.optimization_barrier((two, one))[0]
    three = swap(jnp.where(odd, four, held))

    cut = lambda k: lax.dynamic_slice_in_dim(out_weight, lax.rem(me + k, 4) * cols, cols, axis=1)
    w_own = cut(0)
    w_left = rotated(cut(1), "tp", 1)
    w_right = rotated(cut(3), "tp", -1)
    w_opp = rotated(cut(2), "tp", 2)

    qdoc = doc[:, None]
    iota = jnp.arange(rows, dtype=jnp.int32)
    later = (iota[:, None] > iota[None, :]).astype(BF16)
    lanes = jnp.arange(128, dtype=jnp.int32)
    tri = jnp.where(lanes[:, None] >= lanes[None, :], -1.0, 0.0)
    tri = jnp.concatenate([tri, jnp.full((128, 128), -1.0)], axis=1).astype(BF16)
    tri = jnp.concatenate([tri, tri], axis=0)
    state = attend(True, False, heads, query_rows, (packed,), tri, qdoc, ())
    state = attend(False, False, heads, query_rows, (one, two), tri, qdoc, state)
    state = attend(False, True, heads, query_rows, (three, four), tri, qdoc, state)
    attended = state[0]

    top = expert_ids.shape[1]
    experts = size * gate_weight.shape[0]
    capacity = (4 * rows * top + 3 * experts - 1) // (3 * experts)
    e_iota = jnp.arange(experts, dtype=jnp.int32)[None, :]
    chosen = [(expert_ids[:, k : k + 1] == e_iota) for k in range(top)]
    count = sum(c.astype(BF16) for c in chosen)
    earlier = jnp.dot(later, count, preferred_element_type=F32)
    ids = [expert_ids[:, k : k + 1] for k in range(top)]
    slot = [jnp.sum(jnp.where(c, earlier, 0.0), axis=1, keepdims=True).astype(jnp.int32) for c in chosen]
    targets = jnp.arange(experts * capacity, dtype=jnp.int32)[:, None]
    select = sum((jnp.transpose(i * capacity + s) == targets).astype(BF16) for i, s in zip(ids, slot))

    left, right, opp_t, opp_b = gather_tp(attended)
    opp = jnp.concatenate([opp_t, opp_b], axis=0)
    part = lambda a, w: jnp.dot(a, w, preferred_element_type=F32).astype(BF16).astype(F32)
    projected = part(attended, w_own) + part(left, w_left) + part(right, w_right) + part(opp, w_opp)
    middle = (stream.astype(F32) + projected).astype(BF16)

    tiles = cols // 128
    send = jnp.dot(select, middle, preferred_element_type=F32)
    send = send.astype(BF16).reshape(experts, capacity * tiles, 128)
    block = lax.all_to_all(send, "sp", 0, 0, tiled=True)
    take = lax.rem(jnp.array([0, 3, 1, 2, 2, 1, 3, 0], jnp.int32) + me, 4)
    gain = norm_gain.reshape(4, 1, cols)
    mixed = middle.astype(F32)
    for lo, hi in ((0, 8), (8, capacity)):
        items = hi - lo
        shape = (experts, items, cols) if items % 8 == 0 else (experts, items * tiles, 128)
        part = block[:, lo * tiles : hi * tiles].reshape(experts * items, cols)
        wide = gather_tp(part)
        parts = experts_of(take, part, *wide, gain, gate_weight, up_weight, down_weight)
        result = scatter_sum_tp(parts, shape)
        back = lax.all_to_all(result, "sp", 0, 0, tiled=True).reshape(experts * items, cols)

        slots = jnp.arange(experts * items, dtype=jnp.int32)[None]
        for k in range(top):
            place = jnp.where((slot[k] >= lo) & (slot[k] < hi), ids[k] * items + slot[k] - lo, -1)
            value = jnp.dot((place == slots).astype(BF16), back, preferred_element_type=F32)
            mixed = mixed + value * expert_weights[:, k : k + 1]
    return mixed.astype(BF16)


def solution(mesh):
    in_specs = (
        P("sp", "tp"),
        P("sp", "tp"),
        P("sp", "tp"),
        P("sp", "tp"),
        P("sp"),
        P("tp", None),
        P("sp", "tp"),
        P(),
        P("sp", None),
        P("sp", None),
        P("sp", None, "tp"),
        P("sp", None, "tp"),
        P("sp", "tp", None),
    )
    out_specs = P("sp", "tp")
    return jax.shard_map(layer, mesh=mesh, in_specs=in_specs, out_specs=out_specs, check_vma=False)
```
